32 devices in a mesh: sp: 4 (over z), dp: 8 (over y, x, core).
Axes of the slice: x: 2, y: 2, z: 4, core: 2. Of those that a mesh axis runs over, the one named last changes fastest.
Arguments:
- normed: bfloat16 [8, 512, 2048], P('dp', 'sp'), may hold values from -6 to 6
- values: bfloat16 [8, 512, 2048], P('dp', 'sp'), may hold values from -6 to 6
- gate_in: bfloat16 [8, 512, 2048], P('dp', 'sp'), may hold values from -6 to 6
- step_raw: bfloat16 [8, 512, 32], P('dp', 'sp'), may hold values from -3.5 to 2.5
- upstream: bfloat16 [8, 512, 2048], P('dp', 'sp'), may hold values from -6 to 6
- proj_pair: bfloat16 [2048, 512], P('dp'), may hold values from -0.03125 to 0.03125
- conv_value: float32 [4, 2048], replicated, may hold values from -3 to 3
- conv_pair: float32 [4, 512], replicated, may hold values from -3 to 3
- step_bias: float32 [32], replicated, may hold values from -1 to 1
- decay_log: float32 [32], replicated, may hold values from -12 to -2
- skip: float32 [32], replicated, may hold values from 0.5 to 1.5
Outputs:
- grad_normed: bfloat16 [8, 512, 2048], P('dp', 'sp')
- grad_values: bfloat16 [8, 512, 2048], P('dp', 'sp')
- grad_gate: bfloat16 [8, 512, 2048], P('dp', 'sp')
- grad_step: bfloat16 [8, 512, 32], P('dp', 'sp')
- grad_proj: float32 [2048, 512], P('dp')
The draws below stay inside these ranges and needn't reach their ends.
All inputs are finite; a program needn't handle non-finite values.
Results may differ from the reference program's by a relative error of at most 0.02.
Values may be sent and summed in bfloat16 or wider, within the bound.
A program may use at most 128 MiB of HBM per device.

```python
import math
import jax
import jax.numpy as jnp
from jax import lax

D = 2048
HEADS = 32
HEAD = 64
GROUPS = 2
STATE = 128
TAPS = 4
BLOCK = 64
TOK_DEV = 128
INNER = 2048
LENGTH = 512
BATCH = 8
N_SP = 4


def draw_step_raw(key, part):
    first, second = jax.random.split(jax.random.fold_in(key, 11))
    blocks = LENGTH // TOK_DEV
    shift = jax.random.uniform(first, (BATCH, blocks, 1, HEADS), jnp.float32, -2.0, 1.0)
    noise = jnp.clip(jax.random.normal(second, (BATCH, blocks, TOK_DEV, HEADS), jnp.float32), -3.0, 3.0) * 0.5
    return (shift + noise).reshape(BATCH, LENGTH, HEADS).astype(jnp.bfloat16)


def draw_decay_log(key, part):
    first, second, third = jax.random.split(jax.random.fold_in(key, 23), 3)
    quick_flag = jax.random.randint(first, (HEADS,), 0, 2) == 1
    quick = jnp.exp(jax.random.uniform(second, (HEADS,), jnp.float32, math.log(0.04), math.log(0.12)))
    gentle = jax.random.uniform(third, (HEADS,), jnp.float32, 0.3, 1.0) / LENGTH
    return jnp.log(jnp.where(quick_flag, quick, gentle)).astype(jnp.float32)


def raised(array, own_key, source, target, shards_of, factor):
    def block_of(axis_at):
        return (jnp.arange(array.shape[axis_at]) // (array.shape[axis_at] // shards_of)).reshape((-1,) + (1,) * (array.ndim - 1 - axis_at))

    first = jax.random.permutation(own_key, shards_of)[block_of(target)]
    second = (block_of(target) + shards_of // 2) % shards_of
    return jnp.where((block_of(source) == first) | (block_of(source) == second), factor * array, array)


def block_scale(rng, extent, cuts, least, top_value):
    def one(dim, shards_of):
        heights = jax.random.uniform(jax.random.fold_in(jax.random.fold_in(rng, 6), dim), (shards_of,), jnp.float32, least / len(cuts), top_value / len(cuts))
        return jnp.repeat(jnp.exp(heights), extent[dim] // shards_of).reshape((-1,) + (1,) * (len(extent) - dim - 1))

    level = one(*cuts[0])
    for cut in cuts[1:]:
        level = level * one(*cut)
    return level


def centred(own_key, extent, deviation, bound, pieces=(), kind=jnp.bfloat16):
    loudness = block_scale(own_key, extent, pieces, -0.22, 0.18) if pieces else 1.0
    drawn = jax.random.normal(own_key, extent, jnp.float32) * deviation * loudness
    return jnp.minimum(jnp.maximum(drawn, -bound), bound).astype(kind)


def noise_with(own_key, shape, scale, limit, cuts, heavy, held_as=jnp.bfloat16):
    drawn = scale * jax.random.normal(own_key, shape, jnp.float32)
    if cuts:
        drawn = drawn * block_scale(own_key, shape, cuts, -0.22, 0.18)
    return jnp.clip(raised(drawn, jax.random.fold_in(own_key, 3), *heavy), -limit, limit).astype(held_as)


def setup_inputs(seed: int = 0) -> dict:
    key_list = jax.random.split(jax.random.key(seed), 12)
    normed = noise_with(key_list[0], (BATCH, LENGTH, D), 1.0, 6.0, ((0, 8), (1, 4)), (0, 2, 8, 2.0))
    values = centred(key_list[1], (BATCH, LENGTH, INNER), 1.0, 6.0, ((0, 8), (1, 4)))
    gate_in = centred(key_list[2], (BATCH, LENGTH, INNER), 1.0, 6.0, ((0, 8), (1, 4)))
    step_raw = draw_step_raw(jax.random.fold_in(key_list[11], 71), 0)
    upstream = centred(key_list[4], (BATCH, LENGTH, INNER), 1.0, 6.0, ((0, 8), (1, 4)))
    proj_pair = centred(key_list[5], (D, GROUPS * 2 * STATE), (16 * D) ** -0.5, 0.03125, ((0, 8),))
    conv_value = centred(key_list[6], (TAPS, INNER), TAPS ** -0.5, 3.0, (), jnp.float32)
    conv_pair = centred(key_list[7], (TAPS, GROUPS * 2 * STATE), TAPS ** -0.5, 3.0, (), jnp.float32)
    step_bias = jnp.clip(jax.random.uniform(key_list[8], (HEADS,), jnp.float32, -1.0, 1.0), -1.0, 1.0)
    decay_log = draw_decay_log(jax.random.fold_in(key_list[11], 71), 0)
    skip = jnp.clip(jax.random.uniform(key_list[10], (HEADS,), jnp.float32, 0.5, 1.5), 0.5, 1.5)
    return {"normed": normed, "values": values, "gate_in": gate_in, "step_raw": step_raw, "upstream": upstream, "proj_pair": proj_pair, "conv_value": conv_value, "conv_pair": conv_pair, "step_bias": step_bias, "decay_log": decay_log, "skip": skip}


exact = lax.Precision.HIGHEST

def causal_filter(signal, weights):
    length = signal.shape[0]
    tap_count = weights.shape[0]
    padded = jnp.pad(signal, ((tap_count - 1, 0), (0, 0)))
    summed = jnp.zeros_like(signal)
    for offset in range(tap_count):
        summed = summed + weights[offset] * padded[offset:offset + length]
    return jax.nn.silu(summed)

def silu_slope(gate):
    sig = jax.nn.sigmoid(gate)
    return sig * (1.0 + gate * (1.0 - sig))

def scan_heads(head_value, pair_rows, raw_steps, taps_value, taps_pair, biases, log_rates, skip_gains):
    length, width = head_value.shape
    count = raw_steps.shape[1]
    head_dim = width // count
    state_dim = pair_rows.shape[1] // 2
    blocks = length // BLOCK
    conv_values = causal_filter(head_value, taps_value)
    conv_pairs = causal_filter(pair_rows, taps_pair)
    inject = conv_pairs[:, :state_dim].reshape(blocks, BLOCK, state_dim)
    readout = conv_pairs[:, state_dim:].reshape(blocks, BLOCK, state_dim)
    step_size = jax.nn.softplus(raw_steps + biases[None, :])
    decay_rate = -jnp.exp(log_rates)
    within = jnp.cumsum((step_size * decay_rate[None, :]).reshape(blocks, BLOCK, count), axis=1)
    value_heads = conv_values.reshape(length, count, head_dim)
    scaled = (value_heads * step_size[:, :, None]).reshape(blocks, BLOCK, count, head_dim)
    causal = jnp.tril(jnp.ones((BLOCK, BLOCK), dtype=bool))
    intersect = jnp.einsum('cln,csn->cls', readout, inject, precision=exact)
    spacing = within[:, :, None, :] - within[:, None, :, :]
    weight_diag = jnp.exp(jnp.where(causal[None, :, :, None], spacing, -jnp.inf))
    mixing = intersect[:, :, :, None] * weight_diag
    local_out = jnp.einsum('clsh,cshp->clhp', mixing, scaled, precision=exact)
    to_end = jnp.exp(within[:, -1:, :] - within)
    carried = jnp.einsum('cln,clhp->chpn', inject, scaled * to_end[:, :, :, None], precision=exact)
    block_total = within[:, -1, :]
    running = jnp.cumsum(block_total, axis=0)
    earlier = jnp.tril(jnp.ones((blocks, blocks), dtype=bool), -1)
    link = jnp.exp(jnp.where(earlier[:, :, None], (running - block_total)[:, None, :] - running[None, :, :], -jnp.inf))
    entering = jnp.einsum('cdh,dhpn->chpn', link, carried, precision=exact)
    far_raw = jnp.einsum('cln,chpn->clhp', readout, entering, precision=exact)
    far_out = far_raw * jnp.exp(within)[:, :, :, None]
    direct = (value_heads * skip_gains[None, :, None]).reshape(length, width)
    return (local_out + far_out).reshape(length, width) + direct

def head_grads(head_value, pair_rows, raw_steps, taps_value, taps_pair, biases, log_rates, skip_gains, cotangent):

    def forward(vals, pairs, raws):
        return scan_heads(vals, pairs, raws, taps_value, taps_pair, biases, log_rates, skip_gains)
    output, pullback = jax.vjp(forward, head_value, pair_rows, raw_steps)
    return (output, pullback(cotangent))

def reference(normed, values, gate_in, step_raw, upstream, proj_pair, conv_value, conv_pair, step_bias, decay_log, skip):
    heads_dev = HEADS // N_SP
    width_dev = heads_dev * HEAD
    per_group = N_SP // GROUPS
    pair_width = 2 * STATE
    group_heads = HEADS // GROUPS

    def one_sequence(items):
        token_rows, seq_values, seq_gate, seq_raw, seq_up = items
        pair_pre = jnp.dot(token_rows, proj_pair, preferred_element_type=jnp.float32).astype(jnp.bfloat16)
        gate_float = seq_gate.astype(jnp.float32)
        up_float = seq_up.astype(jnp.float32)
        cot_all = lax.optimization_barrier((up_float * jax.nn.silu(gate_float)).astype(jnp.bfloat16)).astype(jnp.float32)

        def one_device(index):
            first_head = index * heads_dev
            group = first_head // group_heads
            column = first_head * HEAD
            head_value = lax.dynamic_slice_in_dim(seq_values, column, width_dev, 1).astype(jnp.float32)
            pair_rows = lax.dynamic_slice_in_dim(pair_pre, group * pair_width, pair_width, 1).astype(jnp.float32)
            raw_steps = lax.dynamic_slice_in_dim(seq_raw, first_head, heads_dev, 1).astype(jnp.float32)
            taps_value = lax.dynamic_slice_in_dim(conv_value, column, width_dev, 1)
            taps_pair = lax.dynamic_slice_in_dim(conv_pair, group * pair_width, pair_width, 1)
            biases = lax.dynamic_slice_in_dim(step_bias, first_head, heads_dev, 0)
            log_rates = lax.dynamic_slice_in_dim(decay_log, first_head, heads_dev, 0)
            skip_gains = lax.dynamic_slice_in_dim(skip, first_head, heads_dev, 0)
            cotangent = lax.dynamic_slice_in_dim(cot_all, column, width_dev, 1)
            output, grads = head_grads(head_value, pair_rows, raw_steps, taps_value, taps_pair, biases, log_rates, skip_gains, cotangent)
            return (output.astype(jnp.bfloat16), grads[0].astype(jnp.bfloat16), grads[1].astype(jnp.bfloat16), grads[2].astype(jnp.bfloat16))
        outputs, value_grads, pair_grads, step_grads = lax.map(one_device, jnp.arange(N_SP, dtype=jnp.int32))
        side = jnp.moveaxis(outputs, 0, 1).reshape(LENGTH, INNER)
        grad_gate = (up_float * lax.optimization_barrier(side).astype(jnp.float32) * silu_slope(gate_float)).astype(jnp.bfloat16)
        grad_values = jnp.moveaxis(value_grads, 0, 1).reshape(LENGTH, INNER)
        grad_step = jnp.moveaxis(step_grads, 0, 1).reshape(LENGTH, HEADS)
        device_part = lax.optimization_barrier(pair_grads)
        group_sum = device_part.astype(jnp.float32).reshape(GROUPS, per_group, LENGTH, pair_width).sum(axis=1)
        pair_total = jnp.moveaxis(group_sum, 0, 1).reshape(LENGTH, GROUPS * pair_width).astype(jnp.bfloat16)
        grad_normed = lax.dot_general(pair_total, proj_pair, (((1,), (1,)), ((), ())), preferred_element_type=jnp.float32).astype(jnp.bfloat16)
        grad_proj = lax.dot_general(token_rows, pair_total, (((0,), (0,)), ((), ())), preferred_element_type=jnp.float32)
        return (grad_normed, grad_values, grad_gate, grad_step, grad_proj)
    results = lax.map(one_sequence, (normed, values, gate_in, step_raw, upstream))
    return (results[0], results[1], results[2], results[3], lax.optimization_barrier(jnp.sum(results[4], axis=0)))
```

```python
import functools

import jax
import jax.numpy as jnp
from jax import lax
from jax.experimental import pallas as pl
from jax.experimental.pallas import tpu as pltpu
from jax.sharding import PartitionSpec as P

HEAD = 64
STATE = 128
LANES = 128
PAIR = 2 * STATE
exact = lax.Precision.HIGHEST
f32 = jnp.float32
bf16 = jnp.bfloat16

NN = (((1,), (0,)), ((), ()))
NT = (((1,), (1,)), ((), ()))
TN = (((0,), (0,)), ((), ()))


def mm(a, b, dims):
    return lax.dot_general(a, b, dims, preferred_element_type=f32)


def mm_exact(a, b, dims):
    return lax.dot_general(a, b, dims, precision=exact, preferred_element_type=f32)


def mixer_kernel(
    sp,
    heads,
    groups,
    normed,
    values,
    gate,
    up,
    step,
    proj,
    tap_v,
    tap_p,
    bias,
    log_rate,
    skip,
    gn,
    gv,
    gg,
    gs,
    gp,
    cot,
    pair,
    rv,
    rc,
    rs,
    rp,
    xv,
    xp,
    us,
    slope_v,
    slope_p,
    bc,
    xs,
    dxl,
    dbc,
    r1s,
    acs,
    dts,
    sgs,
    st_all,
    st,
    dst_,
    dv,
    dp_,
    ybuf,
    gvbuf,
    gpbuf,
    dtbuf,
    yrec,
    prec,
    drec,
    send_sem,
    recv_sem,
):
    me = lax.axis_index("sp")
    T = values.shape[0]
    inner = values.shape[1]
    W = inner // sp
    hd = heads // sp
    tiles = W // LANES

    barrier = pltpu.get_barrier_semaphore()
    for off in range(1, sp):
        peer = lax.rem(me + off, sp)
        pl.semaphore_signal(
            barrier, inc=1, device_id={"sp": peer}, device_id_type=pl.DeviceIdType.MESH
        )
    pl.semaphore_wait(barrier, sp - 1)

    def rows(i):
        return pl.ds(pl.multiple_of(i * T, T), T)

    def cols(i):
        return pl.ds(pl.multiple_of(i * W, LANES), W)

    def group_cols(i):
        g = (i * hd) // (heads // groups)
        return pl.ds(pl.multiple_of(g * PAIR, LANES), PAIR)

    def remote(kind, src, dst, to, frm):
        return pltpu.make_async_remote_copy(
            src_ref=src,
            dst_ref=dst,
            send_sem=send_sem.at[kind, to],
            recv_sem=recv_sem.at[kind, frm],
            device_id={"sp": to},
            device_id_type=pl.DeviceIdType.MESH,
        )

    def go_values(to, frm):
        return remote(0, values.at[:, cols(to)], rv.at[rows(frm), :], to, frm)

    def go_cot(to, frm):
        return remote(1, cot.at[:, cols(to)], rc.at[rows(frm), :], to, frm)

    def go_step(to, frm):
        return remote(2, step, rs.at[rows(frm), :], to, frm)

    def go_pair(to, frm):
        return remote(3, pair.at[:, group_cols(to)], rp.at[rows(frm), :], to, frm)

    def go_y(to, frm):
        return remote(4, ybuf.at[rows(to), :], yrec.at[:, cols(frm)], to, frm)

    def go_gv(to, frm):
        return remote(5, gvbuf.at[rows(to), :], gv.at[:, cols(frm)], to, frm)

    def go_gp(to, frm):
        return remote(6, gpbuf.at[rows(to), :], prec.at[rows(frm), :], to, frm)

    def go_dt(to, frm):
        return remote(7, dtbuf.at[rows(to), :], drec.at[rows(frm), :], to, frm)

    def send_all(go):
        for off in range(1, sp):
            go(lax.rem(me + off, sp), me).start()

    send_all(go_values)
    send_all(go_step)
    rv[rows(me), :] = values[:, cols(me)]
    rs[rows(me), :] = step[...]

    @pl.loop(0, inner // 256)
    def _(j):
        at = pl.ds(pl.multiple_of(j * 256, 256), 256)
        v = gate[:, at].astype(f32)
        cot[:, at] = (up[:, at].astype(f32) * (v * jax.nn.sigmoid(v))).astype(bf16)

    send_all(go_cot)
    rc[rows(me), :] = cot[:, cols(me)]
    for g in range(groups):
        at = slice(g * PAIR, (g + 1) * PAIR)
        pair[:, at] = mm(normed[...], proj[:, at], NN).astype(bf16)
    send_all(go_pair)
    rp[rows(me), :] = pair[:, group_cols(me)]

    row_i = lax.broadcasted_iota(jnp.int32, (T, T), 0)
    col_i = lax.broadcasted_iota(jnp.int32, (T, T), 1)
    causal = row_i >= col_i
    tri = causal.astype(f32)
    lane = lax.broadcasted_iota(jnp.int32, (T, LANES), 1)
    low = lane < HEAD
    sel_r = lax.broadcasted_iota(jnp.int32, (LANES, W), 0)
    sel_c = lax.broadcasted_iota(jnp.int32, (LANES, W), 1)
    sel = (sel_c // HEAD == sel_r).astype(f32)

    def head_sum(z):
        return mm_exact(z, sel, NT)

    def spread(x, j):
        a = x[:, 2 * j : 2 * j + 1]
        b = x[:, 2 * j + 1 : 2 * j + 2]
        mask = low if x.shape[0] == T else low[0 : x.shape[0]]
        return jnp.where(mask, a, b)

    rate = -jnp.exp(log_rate[...])
    st[...] = jnp.zeros_like(st)
    dst_[...] = jnp.zeros_like(dst_)
    xv[0:8, :] = jnp.zeros((8, W), f32)
    xp[0:8, :] = jnp.zeros((8, PAIR), f32)
    dv[...] = jnp.zeros_like(dv)
    dp_[...] = jnp.zeros_like(dp_)

    def conv(buf, taps, c, at):
        win = buf[pl.ds(pl.multiple_of(c * T, 8), T + 8), at]
        total = taps[0:1, at] * win[5 : 5 + T]
        for k in range(1, 4):
            total = total + taps[k : k + 1, at] * win[5 + k : 5 + k + T]
        return total

    def conv_back(carry, grad, taps, at):
        win = jnp.concatenate([grad, carry[:, at]], axis=0)
        carry[:, at] = grad[0:8]
        total = taps[3:4, at] * win[0:T]
        for k in range(3):
            total = total + taps[k : k + 1, at] * win[3 - k : 3 - k + T]
        return total

    def silu_parts(s):
        sig = jax.nn.sigmoid(s)
        return s * sig, sig * (1.0 + s * (1.0 - sig))

    @pl.loop(0, sp)
    def _(c):
        here = rows(c)
        after8 = pl.ds(pl.multiple_of(c * T + 8, 8), T)

        @pl.when(c != me)
        def _():
            go_values(c, c).wait_recv()
            go_step(c, c).wait_recv()
            go_cot(c, c).wait_recv()
            go_pair(c, c).wait_recv()

        raw = pltpu.roll(rs[here, :].astype(f32), lax.rem(LANES - me * hd, LANES), 1) + bias[...]
        dt = jax.nn.softplus(raw)
        sgs[here, :] = jax.nn.sigmoid(raw)
        dts[here, :] = dt
        ac = mm_exact(tri, dt * rate, NN)
        acs[here, :] = ac
        ac_t = ac.T
        ea = jnp.exp(ac)
        end = ac[T - 1 : T, :]
        te = jnp.exp(end - ac)
        e_end = jnp.exp(end)

        xp[after8, :] = rp[here, :].astype(f32)
        for j in range(2):
            at = slice(j * LANES, (j + 1) * LANES)
            act, slope = silu_parts(conv(xp, tap_p, c, at))
            bc[here, at] = act.astype(bf16)
            slope_p[here, at] = slope
        b = bc[here, 0:STATE]
        cc = bc[here, STATE:PAIR]
        g = mm(cc, b, NT)
        d_g = jnp.zeros((T, T), f32)
        d_c = jnp.zeros((T, STATE), f32)
        zs = []
        for j in range(tiles):
            at = slice(j * LANES, (j + 1) * LANES)
            xv[after8, at] = rv[here, at].astype(f32)
            u, slope = silu_parts(conv(xv, tap_v, c, at))
            us[here, at] = u
            slope_v[here, at] = slope
            dy = rc[here, at]
            x = (u * spread(dt, j)).astype(bf16)
            xs[here, at] = x
            zero = jnp.zeros_like(x)
            decays = []
            mixes = []
            for q in range(2):
                h = 2 * j + q
                diff = ac[:, h : h + 1] - ac_t[h : h + 1, :]
                decay = jnp.exp(jnp.where(causal, diff, -1e30))
                decays.append(decay)
                mixes.append((g * decay).astype(bf16))
            x2 = jnp.concatenate([jnp.where(low, x, zero), jnp.where(low, zero, x)], axis=0)
            dy2 = jnp.concatenate([jnp.where(low, dy, zero), jnp.where(low, zero, dy)], axis=0)
            y = mm(jnp.concatenate(mixes, axis=1), x2, NN)
            dxl[here, at] = mm(jnp.concatenate(mixes, axis=0), dy2, TN)
            d_mix = mm(dy2, x, NT)
            d_g = d_g + d_mix[0:T] * decays[0] + d_mix[T : 2 * T] * decays[1]
            s_in = st[:, at].astype(bf16)
            st_all[pl.ds(pl.multiple_of(c * STATE, STATE), STATE), at] = s_in
            dyf = dy.astype(f32)
            eaj = spread(ea, j)
            y = y + eaj * mm(cc, s_in, NN)
            d_c = d_c + mm((eaj * dyf).astype(bf16), s_in, NT)
            zs.append(dyf * y)
            ybuf[here, at] = (y + spread(skip[...], j) * u).astype(bf16)
            xe = (x.astype(f32) * spread(te, j)).astype(bf16)
            st[:, at] = spread(e_end, j) * st[:, at] + mm(b, xe, TN)
        r1s[here, :] = head_sum(jnp.concatenate(zs, axis=1) if tiles > 1 else zs[0])
        dg = d_g.astype(bf16)
        dbc[here, 0:STATE] = mm(dg, cc, TN)
        dbc[here, STATE:PAIR] = mm(dg, b, NN) + d_c

        @pl.when(c != me)
        def _():
            go_y(c, me).start()

        @pl.when(c == me)
        def _():
            yrec[:, cols(me)] = ybuf[rows(me), :]

    @pl.loop(0, sp)
    def _(i):
        c = sp - 1 - i
        here = rows(c)
        ac = acs[here, :]
        dt = dts[here, :]
        end = ac[T - 1 : T, :]
        ea = jnp.exp(ac)
        te = jnp.exp(end - ac)
        e_end = jnp.exp(end)
        b = bc[here, 0:STATE]
        cc = bc[here, STATE:PAIR]
        d_b = dbc[here, 0:STATE]
        zs = []
        ends = []
        for j in range(tiles):
            at = slice(j * LANES, (j + 1) * LANES)
            ds = dst_[:, at]
            dsb = ds.astype(bf16)
            x = xs[here, at].astype(f32)
            tej = spread(te, j)
            xe = x * tej
            far = mm(b, dsb, NN)
            d_b = d_b + mm(xe.astype(bf16), dsb, NT)
            dx = dxl[here, at] + tej * far
            zs.append(x * dx)
            s_in = st_all[pl.ds(pl.multiple_of(c * STATE, STATE), STATE), at].astype(f32)
            ee = spread(e_end, j)
            ends.append(
                jnp.sum(xe * far, axis=0, keepdims=True)
                + ee * jnp.sum(ds * s_in, axis=0, keepdims=True)
            )
            dyf = rc[here, at].astype(f32)
            du = spread(dt, j) * dx + spread(skip[...], j) * dyf
            gvbuf[here, at] = conv_back(dv, du * slope_v[here, at], tap_v, at).astype(bf16)
            dst_[:, at] = ee * ds + mm(cc, (spread(ea, j) * dyf).astype(bf16), TN)
        z = jnp.concatenate(zs, axis=1) if tiles > 1 else zs[0]
        z_end = jnp.concatenate(ends, axis=1) if tiles > 1 else ends[0]
        xd = head_sum(z)
        d_end = head_sum(jnp.broadcast_to(z_end, (8, W)))[0:1, :]
        d_ac = r1s[here, :] - xd
        back = mm_exact(tri, d_ac, TN) + d_end
        d_dt = (xd / dt + rate * back) * sgs[here, :]
        d_dt = jnp.where(lane < hd, d_dt, 0.0)
        dtbuf[here, :] = pltpu.roll(d_dt, me * hd, 1).astype(bf16)
        for j, part in enumerate((d_b, dbc[here, STATE:PAIR])):
            at = slice(j * LANES, (j + 1) * LANES)
            gpbuf[here, at] = conv_back(dp_, part * slope_p[here, at], tap_p, at).astype(bf16)

        @pl.when(c != me)
        def _():
            go_gp(c, me).start()
            go_gv(c, me).start()
            go_dt(c, me).start()

        @pl.when(c == me)
        def _():
            gv[:, cols(me)] = gvbuf[rows(me), :]
            prec[rows(me), :] = gpbuf[rows(me), :]
            drec[rows(me), :] = dtbuf[rows(me), :]

    def wait_all(go):
        for off in range(1, sp):
            frm = lax.rem(me + off, sp)
            go(frm, frm).wait_recv()

    wait_all(go_y)

    @pl.loop(0, inner // 256)
    def _(j):
        at = pl.ds(pl.multiple_of(j * 256, 256), 256)
        v = gate[:, at].astype(f32)
        sig = jax.nn.sigmoid(v)
        gg[:, at] = (
            up[:, at].astype(f32) * yrec[:, at].astype(f32) * (sig * (1.0 + v * (1.0 - sig)))
        ).astype(bf16)

    wait_all(go_gp)
    totals = []
    for g in range(groups):
        total = None
        for k in range(sp):
            if (k * hd) // (heads // groups) == g:
                term = prec[k * T : (k + 1) * T, :].astype(f32)
                total = term if total is None else total + term
        totals.append(total.astype(bf16))
    dpair = jnp.concatenate(totals, axis=1)
    for j in range(normed.shape[1] // 512):
        at = slice(j * 512, (j + 1) * 512)
        gp[at, :] = mm(normed[:, at], dpair, TN).astype(bf16)
    for j in range(normed.shape[1] // 512):
        at = slice(j * 512, (j + 1) * 512)
        gn[:, at] = mm(dpair, proj[at, :], NT).astype(bf16)
    wait_all(go_dt)
    total = drec[0:T, :].astype(f32)
    for k in range(1, sp):
        total = total + drec[k * T : (k + 1) * T, :].astype(f32)
    gs[...] = total.astype(bf16)
    wait_all(go_gv)
    for go in (go_values, go_cot, go_step, go_pair, go_y, go_gv, go_gp, go_dt):
        for off in range(1, sp):
            to = lax.rem(me + off, sp)
            go(to, me).wait_send()


def per_device(
    normed,
    values,
    gate_in,
    step_raw,
    upstream,
    proj_pair,
    conv_value,
    conv_pair,
    step_bias,
    decay_log,
    skip,
):
    sp = lax.axis_size("sp")
    me = lax.axis_index("sp")
    T = normed.shape[1]
    width = normed.shape[2]
    inner = values.shape[2]
    heads = step_raw.shape[2]
    groups = proj_pair.shape[1] // PAIR
    hd = heads // sp
    W = inner // sp
    L = T * sp
    dp = lax.axis_size("dp")

    def share(block, axis, count):
        copies = jnp.broadcast_to(block[None], (count,) + block.shape)
        return lax.all_to_all(copies, axis, split_axis=0, concat_axis=0, tiled=True)

    full_proj = share(proj_pair, "dp", dp).reshape(-1, proj_pair.shape[1])
    group = (me * hd) // (heads // groups)
    tap_v = lax.dynamic_slice_in_dim(conv_value, me * W, W, 1)
    tap_p = lax.dynamic_slice_in_dim(conv_pair, group * PAIR, PAIR, 1)

    def local(vec):
        part = lax.dynamic_slice_in_dim(vec, me * hd, hd, 0)
        return jnp.pad(part, (0, LANES - hd))[None]

    step = jnp.pad(step_raw[0], ((0, 0), (0, LANES - heads)))
    vmem = pl.BlockSpec(memory_space=pltpu.VMEM)
    V = pltpu.VMEM
    scratch = [
        V((T, inner), bf16),
        V((T, groups * PAIR), bf16),
        V((L, W), bf16),
        V((L, W), bf16),
        V((L, LANES), bf16),
        V((L, PAIR), bf16),
        V((L + 8, W), f32),
        V((L + 8, PAIR), f32),
        V((L, W), f32),
        V((L, W), f32),
        V((L, PAIR), f32),
        V((L, PAIR), bf16),
        V((L, W), bf16),
        V((L, W), f32),
        V((L, PAIR), f32),
        V((L, LANES), f32),
        V((L, LANES), f32),
        V((L, LANES), f32),
        V((L, LANES), f32),
        V((sp * STATE, W), bf16),
        V((STATE, W), f32),
        V((STATE, W), f32),
        V((8, W), f32),
        V((8, PAIR), f32),
        V((L, W), bf16),
        V((L, W), bf16),
        V((L, PAIR), bf16),
        V((L, LANES), bf16),
        V((T, inner), bf16),
        V((L, PAIR), bf16),
        V((L, LANES), bf16),
        pltpu.SemaphoreType.DMA((8, sp)),
        pltpu.SemaphoreType.DMA((8, sp)),
    ]
    gn, gv, gg, gs, gp = pl.pallas_call(
        functools.partial(mixer_kernel, sp, heads, groups),
        out_shape=(
            jax.ShapeDtypeStruct((T, width), bf16),
            jax.ShapeDtypeStruct((T, inner), bf16),
            jax.ShapeDtypeStruct((T, inner), bf16),
            jax.ShapeDtypeStruct((T, LANES), bf16),
            jax.ShapeDtypeStruct((width, groups * PAIR), bf16),
        ),
        in_specs=[vmem] * 11,
        out_specs=(vmem,) * 5,
        scratch_shapes=scratch,
        compiler_params=pltpu.CompilerParams(
            collective_id=0, has_side_effects=True, vmem_limit_bytes=50 * 1024 * 1024
        ),
    )(
        normed[0],
        values[0],
        gate_in[0],
        upstream[0],
        step,
        full_proj,
        tap_v,
        tap_p,
        local(step_bias),
        local(decay_log),
        local(skip),
    )
    terms = lax.all_to_all(
        gp.reshape((dp,) + proj_pair.shape), "dp", split_axis=0, concat_axis=0, tiled=True
    )
    grad_rows = terms.astype(f32).sum(axis=0).astype(bf16)
    grad_proj = share(grad_rows, "sp", sp).astype(f32).sum(axis=0)
    return (gn[None], gv[None], gg[None], gs[None, :, :heads], grad_proj)


def solution(mesh):
    tok = P("dp", "sp", None)
    in_specs = (tok, tok, tok, tok, tok, P("dp", None), P(), P(), P(), P(), P())
    out_specs = (tok, tok, tok, tok, P("dp", None))
    return jax.shard_map(
        per_device, mesh=mesh, in_specs=in_specs, out_specs=out_specs, check_vma=False
    )
```
